32 devices in a mesh: gr: 2 (over x), sp: 8 (over z, y), tp: 2 (over core).
Axes of the slice: x: 2, y: 2, z: 4, core: 2. Of those that a mesh axis runs over, the one named last changes fastest.
Arguments:
- context_input_tensor: bfloat16 [4, 8192, 2048], P(('gr', 'tp'), 'sp'), parts along dimension 0, may hold values from -8 to 8
- content_mapping_matrix: bfloat16 [2048, 1024], replicated, may hold values from -0.125 to 0.125
- address_mapping_matrix: bfloat16 [2048, 256], replicated, may hold values from -0.125 to 0.125
- increment_mapping_matrix: bfloat16 [2048, 16], replicated, may hold values from -0.125 to 0.125
- increment_speed_offset: float32 [16], P('sp'), may hold values from -1 to 0.5
- channel_fading_exponent: float32 [16], P('sp'), may hold values from -12 to -2
- extra_damping_spikes: float32 [4, 16, 8192], P(('gr', 'tp'), 'sp'), parts along dimension 0, may hold values from -3 to 0
- content_smoothing_coefficients: float32 [5, 16, 64], P(None, 'sp'), may hold values from -2.5 to 2.5
- address_smoothing_coefficients: float32 [5, 4, 64], replicated, may hold values from -2.5 to 2.5
- newest_lookup_matrix: bfloat16 [4, 4, 64], P(('gr', 'tp')), parts along dimension 0, may hold values from -6 to 6
- newest_output_switch: bfloat16 [4, 16, 64], P(('gr', 'tp'), 'sp'), parts along dimension 0, may hold values from -6 to 6
- cluster_scaling_coefficients: float32 [16, 64], P('sp'), may hold values from 0.1 to 1.9
Outputs:
- address_content_store: bfloat16 [4, 8192, 16, 128], P(('gr', 'tp'), None, 'sp'), parts along dimension 0
- earliest_switched_retrieval: bfloat16 [4, 16, 64], P(('gr', 'tp'), 'sp'), parts along dimension 0
The draws below stay inside these ranges and needn't reach their ends.
There are 2 independent parts, one for each index of `gr`. The reference program is written for one: setup_inputs(seed, part) draws one part's arguments, and reference() takes and returns one part's arrays. A program takes and returns all parts, laid end to end along the dimension named above; an argument that names none is the same for every part. Nothing has to cross between parts.
All inputs are finite; a program needn't handle non-finite values.
Results may differ from the reference program's by a relative error of at most 0.009.
Values may be sent and summed in bfloat16 or wider, within the bound.
A program may use at most 128 MiB of HBM per device.

```python
import math
import jax
import jax.numpy as jnp
from jax import lax

MODEL = 2048
HEADS = 16
HEAD = 64
GROUPS = 4
STATE = 64
KERNEL = 5
SPAN = 1024
SEQS = 2
LEN = 8192


def draw_context_input_tensor(key, part):
    key_base, key_scale = jax.random.split(jax.random.fold_in(key, 11))
    normal_part = jnp.clip(jax.random.normal(key_base, (SEQS, LEN, MODEL), jnp.float32), -4.0, 4.0)
    block_scale = jnp.exp(jax.random.uniform(key_scale, (SEQS, LEN // SPAN, 1, 1), jnp.float32, math.log(0.5), math.log(2.0)))
    shaped = normal_part.reshape(SEQS, LEN // SPAN, SPAN, MODEL) * block_scale
    return shaped.reshape(SEQS, LEN, MODEL).astype(jnp.bfloat16)


def draw_channel_fading_exponent(key, part):
    key_order, key_slow, key_fast = jax.random.split(jax.random.fold_in(key, 23), 3)
    ranking = jax.random.permutation(key_order, HEADS)
    slow_rate = jax.random.uniform(key_slow, (HEADS,), jnp.float32, 0.3, 1.5) / LEN
    fast_rate = jnp.exp(jax.random.uniform(key_fast, (HEADS,), jnp.float32, math.log(0.015), math.log(0.05)))
    fast_count = HEADS // 2
    chosen = jnp.where(ranking < fast_count, fast_rate, slow_rate)
    return jnp.log(chosen).astype(jnp.float32)


def draw_extra_damping_spikes(key, part):
    key_place, key_depth = jax.random.split(jax.random.fold_in(key, 37))
    places = jax.random.randint(key_place, (SEQS, 4), 0, LEN)
    depths = jnp.log(1.0 - jax.random.uniform(key_depth, (SEQS, 4), jnp.float32, 0.2, 0.5))
    positions = jnp.arange(LEN, dtype=jnp.int32)
    matches = (positions[None, None, :] == places[:, :, None]).astype(jnp.float32)
    summed = jnp.sum(matches * depths[:, :, None], axis=1)
    return jnp.broadcast_to(summed[:, None, :], (SEQS, HEADS, LEN)).astype(jnp.float32)


def block_levels(rng, dims, cuts, smallest, top_value):
    loudness = 1.0
    for dim, blocks in cuts:
        draws = jax.random.uniform(jax.random.fold_in(jax.random.fold_in(rng, 6), dim), (blocks,), jnp.float32, smallest / len(cuts), top_value / len(cuts))
        loudness = loudness * jnp.repeat(jnp.exp(draws), dims[dim] // blocks).reshape((-1,) + (1,) * (len(dims) - 1 - dim))
    return loudness


def normal_values(own_key, dims, scale, reach, pieces=(), kind=jnp.bfloat16):
    values = scale * jax.random.normal(own_key, dims, jnp.float32)
    if pieces:
        values = values * block_levels(own_key, dims, pieces, -0.22, 0.18)
    return jnp.clip(values, -reach, reach).astype(kind)


def setup_inputs(seed: int = 0, part: int = 0) -> dict:
    arg_keys = jax.random.split(jax.random.key(seed), 13)
    own_keys = jax.random.split(jax.random.fold_in(arg_keys[12], part), 13)
    return {
        "context_input_tensor": draw_context_input_tensor(jax.random.fold_in(jax.random.fold_in(arg_keys[12], part), 71), part),
        "content_mapping_matrix": normal_values(arg_keys[1], (MODEL, HEADS * HEAD), MODEL ** -0.5, 0.125),
        "address_mapping_matrix": normal_values(arg_keys[2], (MODEL, GROUPS * STATE), MODEL ** -0.5, 0.125),
        "increment_mapping_matrix": normal_values(arg_keys[3], (MODEL, HEADS), MODEL ** -0.5, 0.125),
        "increment_speed_offset": jnp.clip(-1.0 + 1.5 * jax.random.uniform(arg_keys[4], (HEADS,), jnp.float32) ** block_levels(arg_keys[4], (HEADS,), ((0, 8),), -0.2, 0.2), -1.0, 0.5),
        "channel_fading_exponent": draw_channel_fading_exponent(jax.random.fold_in(arg_keys[12], 71), part),
        "extra_damping_spikes": draw_extra_damping_spikes(jax.random.fold_in(jax.random.fold_in(arg_keys[12], part), 71), part),
        "content_smoothing_coefficients": normal_values(arg_keys[7], (KERNEL, HEADS, HEAD), KERNEL ** -0.5, 2.5, ((1, 8),), jnp.float32),
        "address_smoothing_coefficients": normal_values(arg_keys[8], (KERNEL, GROUPS, STATE), KERNEL ** -0.5, 2.5, (), jnp.float32),
        "newest_lookup_matrix": normal_values(own_keys[9], (SEQS, GROUPS, STATE), 1.0, 6.0, ((0, 2),)),
        "newest_output_switch": normal_values(own_keys[10], (SEQS, HEADS, HEAD), 1.0, 6.0, ((0, 2), (1, 8))),
        "cluster_scaling_coefficients": jnp.clip(1.0 + 0.18 * jax.random.normal(arg_keys[11], (HEADS, HEAD), jnp.float32), 0.1, 1.9),
    }


EPS = 1e-05

def centred(signal, kernel):
    margin = kernel.shape[0] // 2
    length = signal.shape[0]
    padded = jnp.pad(signal, ((margin, margin), (0, 0), (0, 0)))
    summed = kernel[0] * padded[0:length]
    for offset in range(1, kernel.shape[0]):
        summed = summed + kernel[offset] * padded[offset:offset + length]
    return summed

def reference(context_input_tensor, content_mapping_matrix, address_mapping_matrix, increment_mapping_matrix, increment_speed_offset, channel_fading_exponent, extra_damping_spikes, content_smoothing_coefficients, address_smoothing_coefficients, newest_lookup_matrix, newest_output_switch, cluster_scaling_coefficients):
    repeats = HEADS // GROUPS

    def lone_context_series(packed_buffer):
        prompt_token_rows, arrival_token_rows, query_vector_row, gate_vector_row = packed_buffer
        value_proj = jnp.dot(prompt_token_rows, content_mapping_matrix, preferred_element_type=jnp.float32).astype(jnp.bfloat16).reshape(LEN, HEADS, HEAD)
        key_proj = jnp.dot(prompt_token_rows, address_mapping_matrix, preferred_element_type=jnp.float32).astype(jnp.bfloat16).reshape(LEN, GROUPS, STATE)
        rate_raw = jnp.dot(prompt_token_rows, increment_mapping_matrix, preferred_element_type=jnp.float32).astype(jnp.bfloat16)
        value_conv = jax.nn.silu(centred(value_proj.astype(jnp.float32), content_smoothing_coefficients)).astype(jnp.bfloat16)
        key_conv = jax.nn.silu(centred(key_proj.astype(jnp.float32), address_smoothing_coefficients)).astype(jnp.bfloat16)
        key_heads = jnp.repeat(key_conv, repeats, axis=1)
        smoothed_increment_speed = jax.nn.softplus(rate_raw.astype(jnp.float32) + increment_speed_offset)
        exponent_increment_amount = -jnp.exp(channel_fading_exponent) * smoothed_increment_speed + arrival_token_rows.T
        cumul = jnp.cumsum(exponent_increment_amount, axis=0)
        end_weight = jnp.exp(cumul[-1] - cumul)
        weighted = (value_conv.astype(jnp.float32) * (smoothed_increment_speed * end_weight)[:, :, None]).astype(jnp.bfloat16)
        states = jnp.einsum('lhp,lhn->hpn', weighted.astype(jnp.float32), key_heads.astype(jnp.float32))
        query_heads = jnp.repeat(query_vector_row.astype(jnp.float32), repeats, axis=0)
        raw_read = jnp.einsum('hpn,hn->hp', states, query_heads, precision=lax.Precision.HIGHEST)
        gated_read = raw_read * jax.nn.silu(gate_vector_row.astype(jnp.float32))
        head_sq = lax.optimization_barrier(jnp.sum(gated_read * gated_read, axis=1))
        group_sq = jnp.repeat(lax.optimization_barrier(jnp.sum(head_sq.reshape(GROUPS, repeats), axis=1)), repeats)
        scaled = gated_read * lax.rsqrt(group_sq / (repeats * HEAD) + EPS)[:, None] * cluster_scaling_coefficients
        kv_rows = jnp.concatenate([value_conv, key_heads], axis=-1)
        return (kv_rows, scaled.astype(jnp.bfloat16))
    address_content_store, earliest_switched_retrieval = lax.map(lone_context_series, (context_input_tensor, extra_damping_spikes, newest_lookup_matrix, newest_output_switch))
    return (address_content_store, earliest_switched_retrieval)
```

```python
import functools

import jax
import jax.numpy as jnp
from jax import lax
from jax.experimental import pallas as pl
from jax.experimental.pallas import tpu as pltpu
from jax.sharding import PartitionSpec as P

HEADS = 16
HEAD = 64
GROUPS = 4
STATE = 64
KERNEL = 5
GROUP_HEADS = HEADS // GROUPS


EPS = 1e-05


def swapped(value, axis, bit):
    mask = 2**bit
    pairs = [(source, source ^ mask) for source in range(lax.axis_size(axis))]
    return lax.ppermute(value, axis, pairs)


def centred(signal, kernel):
    margin = kernel.shape[0] // 2
    length = signal.shape[0]
    padded = jnp.pad(signal, ((margin, margin), (0, 0), (0, 0)))
    summed = kernel[0] * padded[0:length]
    for offset in range(1, kernel.shape[0]):
        summed = summed + kernel[offset] * padded[offset : offset + length]
    return summed


def on_device(
    context_input_tensor,
    content_mapping_matrix,
    address_mapping_matrix,
    increment_mapping_matrix,
    increment_speed_offset,
    channel_fading_exponent,
    extra_damping_spikes,
    content_smoothing_coefficients,
    address_smoothing_coefficients,
    newest_lookup_matrix,
    newest_output_switch,
    cluster_scaling_coefficients,
):
    prompt_token_rows = context_input_tensor[0]
    span_len = prompt_token_rows.shape[0]
    repeats = HEADS // GROUPS
    local_heads = increment_speed_offset.shape[0]
    group_devices = repeats // local_heads
    group_index = lax.axis_index("sp") * local_heads // repeats
    value_proj = (
        jnp.dot(prompt_token_rows, content_mapping_matrix, preferred_element_type=jnp.float32)
        .astype(jnp.bfloat16)
        .reshape(span_len, HEADS, HEAD)
    )
    key_proj = (
        jnp.dot(prompt_token_rows, address_mapping_matrix, preferred_element_type=jnp.float32)
        .astype(jnp.bfloat16)
        .reshape(span_len, GROUPS, STATE)
    )
    rate_raw = jnp.dot(
        prompt_token_rows, increment_mapping_matrix, preferred_element_type=jnp.float32
    ).astype(jnp.bfloat16)
    key_copies = jnp.repeat(key_proj, repeats, axis=1)
    value_seq, key_seq, rate_seq = (
        lax.all_to_all(value_proj, "sp", split_axis=1, concat_axis=0, tiled=True),
        lax.all_to_all(key_copies, "sp", split_axis=1, concat_axis=0, tiled=True),
        lax.all_to_all(rate_raw, "sp", split_axis=1, concat_axis=0, tiled=True),
    )
    key_group = key_seq[:, 0:1]
    seq_len = value_seq.shape[0]
    kernel_key = lax.dynamic_slice_in_dim(address_smoothing_coefficients, group_index, 1, 1)
    value_conv = jax.nn.silu(
        centred(value_seq.astype(jnp.float32), content_smoothing_coefficients)
    ).astype(jnp.bfloat16)
    key_conv = jax.nn.silu(centred(key_group.astype(jnp.float32), kernel_key)).astype(jnp.bfloat16)
    key_heads = jnp.broadcast_to(key_conv, (seq_len, local_heads, STATE))
    smoothed_increment_speed = jax.nn.softplus(
        rate_seq.astype(jnp.float32) + increment_speed_offset
    )
    exponent_increment_amount = (
        -jnp.exp(channel_fading_exponent) * smoothed_increment_speed + extra_damping_spikes[0].T
    )
    cumul = jnp.cumsum(exponent_increment_amount, axis=0)
    end_weight = jnp.exp(cumul[-1] - cumul)
    weighted = (
        value_conv.astype(jnp.float32) * (smoothed_increment_speed * end_weight)[:, :, None]
    ).astype(jnp.bfloat16)
    states = jnp.einsum("lhp,lhn->hpn", weighted, key_heads, preferred_element_type=jnp.float32)
    query_vector_row = lax.dynamic_slice_in_dim(newest_lookup_matrix[0], group_index, 1, 0).astype(
        jnp.float32
    )
    query_heads = jnp.broadcast_to(query_vector_row, (local_heads, STATE))
    raw_read = jnp.einsum("hpn,hn->hp", states, query_heads, precision=lax.Precision.HIGHEST)
    gated_read = raw_read * jax.nn.silu(newest_output_switch[0].astype(jnp.float32))
    group_sq = jnp.sum(gated_read * gated_read).reshape(1)
    for level in range(group_devices.bit_length() - 1):
        group_sq = group_sq + swapped(group_sq, "sp", level)
    scaled = (
        gated_read * lax.rsqrt(group_sq[0] / (repeats * HEAD) + EPS) * cluster_scaling_coefficients
    )
    kv_rows = jnp.concatenate([value_conv, key_heads], axis=-1)
    return (kv_rows[None], scaled.astype(jnp.bfloat16)[None])


XLANES = 128
MASKS = (2, 3, 1, 0)
HALO = 16
MESH = pl.DeviceIdType.MESH


def flipped(index, mask):
    total = 0
    for bit in range(2):
        digit = (index // 2**bit) % 2
        total = total + 2**bit * ((1 - digit) if (mask >> bit) & 1 else digit)
    return total


def mixer_kernel(
    n,
    x_hbm,
    wv_hbm,
    wk_hbm,
    wr_ref,
    offset_ref,
    fade_ref,
    spikes_ref,
    taps_ref,
    key_taps_ref,
    query_ref,
    gate_ref,
    gain_ref,
    rows_out,
    read_out,
    x_ext,
    wv,
    wk,
    proj,
    taps_all,
    key_send,
    key_recv,
    value_send,
    value_recv,
    rate_send,
    rate_recv,
    rate_rows,
    spike_rows,
    weights,
    acc,
    mixed,
    packed,
    square_send,
    square_recv,
    load_sem,
    halo_send_sem,
    halo_recv_sem,
    taps_send_sem,
    taps_recv_sem,
    rate_send_sem,
    rate_recv_sem,
    key_send_sem,
    key_recv_sem,
    forward_sem,
    value_send_sem,
    value_recv_sem,
    square_sem,
    out_sem,
):
    span = x_hbm.shape[0]
    half = span // 2
    rows_ext = span + 2 * HALO
    me = lax.axis_index("sp")
    z, y = me // 2, me % 2
    partner = 2 * z + 1 - y
    chunk = 128
    chunks = span // chunk

    def remote(src, dst, send, recv, device):
        return pltpu.make_async_remote_copy(
            src_ref=src,
            dst_ref=dst,
            send_sem=send,
            recv_sem=recv,
            device_id={"sp": device},
            device_id_type=MESH,
        )

    load_x = pltpu.make_async_copy(x_hbm, x_ext.at[pl.ds(HALO, span)], load_sem.at[0])
    load_x.start()
    load_k = pltpu.make_async_copy(wk_hbm, wk, load_sem.at[1])
    load_k.start()
    groups = [flipped(z, mask) for mask in MASKS]
    load_v = []
    for step, group in enumerate(groups):
        columns = pl.ds(pl.multiple_of(group * 256, 256), 256)
        load_v.append(
            pltpu.make_async_copy(wv_hbm.at[:, columns], wv.at[step], load_sem.at[2 + step])
        )
        load_v[-1].start()

    barrier = pltpu.get_barrier_semaphore()
    for hop in range(1, n):
        pl.semaphore_signal(
            barrier, inc=1, device_id={"sp": (me + hop) % n}, device_id_type=MESH
        )
    own_taps = jnp.concatenate([taps_ref[:, 0, :], taps_ref[:, 1, :]], axis=1)
    taps_all[me] = jnp.concatenate([own_taps, jnp.zeros((3, XLANES), jnp.float32)], axis=0)
    pl.semaphore_wait(barrier, n - 1)

    copies = []
    after, before = (me + 1) % n, (me + n - 1) % n
    halo_down = remote(
        x_hbm.at[pl.ds(span - HALO, HALO)],
        x_ext.at[pl.ds(0, HALO)],
        halo_send_sem.at[0],
        halo_recv_sem.at[0],
        after,
    )
    halo_up = remote(
        x_hbm.at[pl.ds(0, HALO)],
        x_ext.at[pl.ds(span + HALO, HALO)],
        halo_send_sem.at[1],
        halo_recv_sem.at[1],
        before,
    )
    halo_down.start()
    halo_up.start()
    for hop in range(1, n):
        copy = remote(
            taps_all.at[me],
            taps_all.at[me],
            taps_send_sem.at[hop],
            taps_recv_sem.at[me],
            (me + hop) % n,
        )
        copy.start()
        copies.append(copy)

    load_x.wait()
    raw = jnp.dot(
        x_ext[HALO : HALO + span, :], wr_ref[...], preferred_element_type=jnp.float32
    )
    raw = raw.astype(jnp.bfloat16).astype(jnp.float32).T
    for device in range(n):
        rate_send[device] = raw[2 * device : 2 * device + 2]
    rate_recv[me] = rate_send[me]
    for hop in range(1, n):
        other = (me + hop) % n
        copy = remote(
            rate_send.at[other],
            rate_recv.at[me],
            rate_send_sem.at[hop],
            rate_recv_sem.at[me],
            other,
        )
        copy.start()
        copies.append(copy)

    halo_down.wait_recv()
    halo_up.wait_recv()

    @pl.when(me == 0)
    def _():
        x_ext[0:HALO, :] = jnp.zeros((HALO, x_ext.shape[1]), jnp.bfloat16)

    @pl.when(me == n - 1)
    def _():
        x_ext[span + HALO :, :] = jnp.zeros((HALO, x_ext.shape[1]), jnp.bfloat16)

    def project(weight):
        piece = rows_ext // 2

        @pl.loop(0, 2)
        def _(index):
            rows = pl.ds(pl.multiple_of(index * piece, 16), piece)
            proj[rows, :] = (
                jnp.dot(x_ext[rows, :], weight[...], preferred_element_type=jnp.float32)
                .astype(jnp.bfloat16)
                .astype(jnp.float32)
            )

    def smooth(index, taps):
        window = proj[pl.ds(pl.multiple_of(index * chunk + 8, 8), chunk + 16), :]
        summed = taps[0:1] * window[6 : 6 + chunk]
        for tap in range(1, KERNEL):
            summed = summed + taps[tap : tap + 1] * window[6 + tap : 6 + tap + chunk]
        return summed * jax.nn.sigmoid(summed)

    load_k.wait()
    project(wk)
    key_taps = jnp.concatenate([key_taps_ref[:, g, :] for g in range(GROUPS)], axis=1)
    lane = lax.broadcasted_iota(jnp.int32, (chunk, XLANES), 1)

    @pl.loop(0, chunks // 2)
    def _(index):
        first = smooth(index, key_taps)
        second = smooth(index + chunks // 2, key_taps)
        rows = pl.ds(pl.multiple_of(index * chunk, chunk), chunk)
        for pair in range(2):
            low = first[:, pair * XLANES : (pair + 1) * XLANES]
            high = second[:, pair * XLANES : (pair + 1) * XLANES]
            key_send[2 * pair, rows, :] = jnp.where(
                lane < 64, low, pltpu.roll(high, 64, 1)
            ).astype(jnp.bfloat16)
            key_send[2 * pair + 1, rows, :] = jnp.where(
                lane < 64, pltpu.roll(low, 64, 1), high
            ).astype(jnp.bfloat16)

    for step in range(3):
        copy = remote(
            key_send.at[groups[step]],
            key_recv.at[me],
            key_send_sem.at[step],
            key_recv_sem.at[me],
            2 * groups[step] + y,
        )
        copy.start()
        copies.append(copy)
    own_forward = remote(
        key_send.at[z], key_recv.at[me], forward_sem.at[3], key_recv_sem.at[me], partner
    )
    own_forward.start()
    copies.append(own_forward)
    key_recv[me] = key_send[z]

    for hop in range(1, n):
        source = (me + hop) % n
        remote(
            taps_all.at[source],
            taps_all.at[source],
            taps_send_sem.at[hop],
            taps_recv_sem.at[source],
            source,
        ).wait_recv()

    for step, group in enumerate(groups):
        load_v[step].wait()
        project(wv.at[step])
        taps = jnp.concatenate([taps_all[2 * group], taps_all[2 * group + 1]], axis=1)

        @pl.loop(0, chunks)
        def _(index):
            value = smooth(index, taps).astype(jnp.bfloat16)
            rows = pl.ds(pl.multiple_of(index * chunk, chunk), chunk)
            value_send[step, 0, rows, :] = value[:, :XLANES]
            value_send[step, 1, rows, :] = value[:, XLANES:]

        for side in range(2):
            if step < 3:
                copy = remote(
                    value_send.at[step, side],
                    value_recv.at[me],
                    value_send_sem.at[step, side],
                    value_recv_sem.at[me],
                    2 * group + side,
                )
                copy.start()
                copies.append(copy)
    last = remote(
        value_send.at[3, 1 - y],
        value_recv.at[me],
        value_send_sem.at[3, 0],
        value_recv_sem.at[me],
        partner,
    )
    last.start()
    copies.append(last)
    value_recv[me] = value_send[3, y]

    for hop in range(1, n):
        source = (me + hop) % n
        remote(
            rate_send.at[source],
            rate_recv.at[source],
            rate_send_sem.at[hop],
            rate_recv_sem.at[source],
            source,
        ).wait_recv()
    for source in range(n):
        rate_rows[2 * source : 2 * source + 2, :] = rate_recv[source]
        spike_rows[2 * source : 2 * source + 2, :] = spikes_ref[
            :, source * span : (source + 1) * span
        ]
    full = (2 * n, span)
    odd = lax.broadcasted_iota(jnp.int32, full, 0) % 2 == 1
    position = lax.broadcasted_iota(jnp.int32, full, 1)
    shifted = rate_rows[...] + jnp.where(odd, offset_ref[1], offset_ref[0])
    rate = jnp.maximum(shifted, 0.0) + jnp.log1p(jnp.exp(-jnp.abs(shifted)))
    decay = jnp.exp(jnp.where(odd, fade_ref[1], fade_ref[0]))
    later = spike_rows[...] - decay * rate
    reach = 1
    while reach < span:
        later = later + jnp.where(
            position < span - reach, pltpu.roll(later, span - reach, 1), 0.0
        )
        reach *= 2
    blocks = jnp.broadcast_to(later[:, 0:1], (2 * n, XLANES))
    block_row = lax.broadcasted_iota(jnp.int32, (2 * n, XLANES), 0)
    reach = 2
    while reach < 2 * n:
        blocks = blocks + jnp.where(
            block_row < 2 * n - reach, pltpu.roll(blocks, 2 * n - reach, 0), 0.0
        )
        reach *= 2
    blocks = jnp.where(block_row < 2 * n - 2, pltpu.roll(blocks, 2 * n - 2, 0), 0.0)
    later = jnp.where(position < span - 1, pltpu.roll(later, span - 1, 1), 0.0)
    scaled = rate * jnp.exp(later + blocks[:, 0:1])
    for source in range(n):
        weights[source] = scaled[2 * source : 2 * source + 2]

    queries = query_ref[...].astype(jnp.float32)
    query_row = lax.broadcasted_iota(jnp.int32, queries.shape, 0)
    query = jnp.sum(jnp.where(query_row == z, queries, 0.0), axis=0, keepdims=True)
    blank = jnp.zeros((1, 64), jnp.float32)
    asked = jnp.concatenate(
        [
            jnp.concatenate([query, blank], axis=1),
            jnp.concatenate([blank, query], axis=1),
            jnp.zeros((6, XLANES), jnp.float32),
        ],
        axis=0,
    ).astype(jnp.bfloat16)
    acc[...] = jnp.zeros_like(acc)

    def take(source, slot):
        scores = lax.dot_general(
            asked,
            key_recv[source],
            (((1,), (1,)), ((), ())),
            preferred_element_type=jnp.float32,
        )
        share = weights[source] * jnp.concatenate([scores[0:1], scores[1:2]], axis=1)
        high = share.astype(jnp.bfloat16).astype(jnp.float32)
        parts = jnp.concatenate(
            [high, share - high, jnp.zeros((4, span), jnp.float32)], axis=0
        ).astype(jnp.bfloat16)
        acc[...] += jnp.dot(parts, value_recv[source], preferred_element_type=jnp.float32)

        for part in range(2):

            @pl.loop(0, chunks // 2)
            def _(index):
                at = pl.multiple_of(index * chunk, chunk)
                value = value_recv[source, pl.ds(part * half + at, chunk), :].astype(jnp.float32)
                key = key_recv[source, pl.ds(at, chunk), :].astype(jnp.float32)
                if part == 0:
                    key = pltpu.roll(key, 64, 1)
                mixed[pl.ds(0, chunk, stride=2), :] = jnp.where(lane < 64, value, key)
                mixed[pl.ds(1, chunk, stride=2), :] = jnp.where(
                    lane < 64, pltpu.roll(value, 64, 1), key
                )
                packed[slot, pl.ds(2 * (part * half + at), 2 * chunk), :] = mixed[...].astype(
                    jnp.bfloat16
                )

        out = pltpu.make_async_copy(
            packed.at[slot],
            rows_out.at[pl.ds(pl.multiple_of(source * 2 * span, 2 * span), 2 * span)],
            out_sem.at[slot],
        )
        out.start()
        return out

    def key_wait(source):
        remote(
            key_recv.at[source],
            key_recv.at[source],
            forward_sem.at[0],
            key_recv_sem.at[source],
            partner,
        ).wait_recv()

    for step in range(3):
        source = 2 * groups[step] + y
        key_wait(source)
        copy = remote(
            key_recv.at[source],
            key_recv.at[source],
            forward_sem.at[step],
            key_recv_sem.at[source],
            partner,
        )
        copy.start()
        copies.append(copy)

    order = [(me, False, False), (partner, True, True)]
    for step in range(3):
        order.append((2 * groups[step] + y, False, True))
        order.append((2 * groups[step] + 1 - y, True, True))
    outs = []
    for index, (source, wait_key, wait_value) in enumerate(order):
        if wait_key:
            key_wait(source)
        if wait_value:
            remote(
                value_recv.at[source],
                value_recv.at[source],
                value_send_sem.at[0, 0],
                value_recv_sem.at[source],
                source,
            ).wait_recv()
        if index >= 2:
            outs[index - 2].wait()
        outs.append(take(source, index % 2))

    total = acc[...]
    first, second = total[0:1] + total[2:3], total[1:2] + total[3:4]
    line = lax.broadcasted_iota(jnp.int32, (1, XLANES), 1)
    raw_read = jnp.where(line < 64, first, second)
    gate = gate_ref[...].astype(jnp.float32)
    gate = jnp.concatenate([gate[0:1], gate[1:2]], axis=1)
    gain = gain_ref[...]
    gain = jnp.concatenate([gain[0:1], gain[1:2]], axis=1)
    gated = raw_read * (gate * jax.nn.sigmoid(gate))
    square = jnp.sum(gated * gated, axis=1, keepdims=True)
    square_send[...] = jnp.broadcast_to(square, square_send.shape)
    swap = remote(square_send, square_recv, square_sem.at[0], square_sem.at[1], partner)
    swap.start()
    swap.wait()
    both = square + square_recv[0:1, 0:1]
    result = gated * lax.rsqrt(both / (GROUP_HEADS * HEAD) + EPS) * gain
    read_out[0:1, :] = result[:, :64]
    read_out[1:2, :] = result[:, 64:]

    outs[-2].wait()
    outs[-1].wait()
    halo_down.wait_send()
    halo_up.wait_send()
    for copy in copies:
        copy.wait_send()


def on_device_kernel(n, *arguments):
    x, wv, wk, wr, offset, fade, spikes, taps, key_taps, query, gate, gain = arguments
    span, model = x.shape[1:]
    f32, bf16 = jnp.float32, jnp.bfloat16
    vmem = pl.BlockSpec(memory_space=pltpu.VMEM)
    smem = pl.BlockSpec(memory_space=pltpu.SMEM)
    anywhere = pl.BlockSpec(memory_space=pl.ANY)
    dma = pltpu.SemaphoreType.DMA
    rows, read = pl.pallas_call(
        functools.partial(mixer_kernel, n),
        out_shape=(
            jax.ShapeDtypeStruct((n * span * 2, 128), bf16),
            jax.ShapeDtypeStruct((2, HEAD), f32),
        ),
        in_specs=[anywhere] * 3 + [vmem] + [smem] * 2 + [vmem] * 6,
        out_specs=(anywhere, vmem),
        scratch_shapes=[
            pltpu.VMEM((span + 2 * HALO, model), bf16),
            pltpu.VMEM((4, model, 256), bf16),
            pltpu.VMEM((model, 256), bf16),
            pltpu.VMEM((span + 2 * HALO, 256), f32),
            pltpu.VMEM((n, 8, 128), f32),
            pltpu.VMEM((GROUPS, span // 2, 128), bf16),
            pltpu.VMEM((n, span // 2, 128), bf16),
            pltpu.VMEM((4, 2, span, 128), bf16),
            pltpu.VMEM((n, span, 128), bf16),
            pltpu.VMEM((n, 2, span), f32),
            pltpu.VMEM((n, 2, span), f32),
            pltpu.VMEM((2 * n, span), f32),
            pltpu.VMEM((2 * n, span), f32),
            pltpu.VMEM((n, 2, span), f32),
            pltpu.VMEM((8, 128), f32),
            pltpu.VMEM((256, 128), f32),
            pltpu.VMEM((2, 2 * span, 128), bf16),
            pltpu.VMEM((8, 128), f32),
            pltpu.VMEM((8, 128), f32),
            dma((6,)),
            dma((2,)),
            dma((2,)),
            dma((n,)),
            dma((n,)),
            dma((n,)),
            dma((n,)),
            dma((3,)),
            dma((n,)),
            dma((4,)),
            dma((4, 2)),
            dma((n,)),
            dma((2,)),
            dma((2,)),
        ],
        compiler_params=pltpu.CompilerParams(
            collective_id=0, has_side_effects=True, vmem_limit_bytes=48 * 2**20
        ),
    )(x[0], wv, wk, wr, offset, fade, spikes[0], taps, key_taps, query[0], gate[0], gain)
    return rows.reshape(1, n * span, 2, 2 * HEAD), read.astype(bf16)[None]


def solution(mesh):
    placed = (
        P(("gr", "tp"), "sp", None),
        P(),
        P(),
        P(),
        P("sp"),
        P("sp"),
        P(("gr", "tp"), "sp", None),
        P(None, "sp", None),
        P(),
        P(("gr", "tp"), None, None),
        P(("gr", "tp"), "sp", None),
        P("sp", None),
    )
    devices = mesh.shape["sp"]
    pairs = HEADS == 2 * devices and GROUPS * 2 == devices
    return jax.shard_map(
        functools.partial(on_device_kernel, devices) if pairs else on_device,
        mesh=mesh,
        in_specs=placed,
        out_specs=(P(("gr", "tp"), None, "sp", None), P(("gr", "tp"), "sp", None)),
        check_vma=False,
    )
```

```python
import functools

import jax
import jax.numpy as jnp
from jax import lax
from jax.experimental import pallas as pl
from jax.experimental.pallas import tpu as pltpu
from jax.sharding import PartitionSpec as P

HEADS = 16
HEAD = 64
GROUPS = 4
STATE = 64
KERNEL = 5
GROUP_HEADS = HEADS // GROUPS


EPS = 1e-05


def swapped(value, axis, bit):
    mask = 2**bit
    pairs = [(source, source ^ mask) for source in range(lax.axis_size(axis))]
    return lax.ppermute(value, axis, pairs)


def centred(signal, kernel):
    margin = kernel.shape[0] // 2
    length = signal.shape[0]
    padded = jnp.pad(signal, ((margin, margin), (0, 0), (0, 0)))
    summed = kernel[0] * padded[0:length]
    for offset in range(1, kernel.shape[0]):
        summed = summed + kernel[offset] * padded[offset : offset + length]
    return summed


def on_device(
    context_input_tensor,
    content_mapping_matrix,
    address_mapping_matrix,
    increment_mapping_matrix,
    increment_speed_offset,
    channel_fading_exponent,
    extra_damping_spikes,
    content_smoothing_coefficients,
    address_smoothing_coefficients,
    newest_lookup_matrix,
    newest_output_switch,
    cluster_scaling_coefficients,
):
    prompt_token_rows = context_input_tensor[0]
    span_len = prompt_token_rows.shape[0]
    repeats = HEADS // GROUPS
    local_heads = increment_speed_offset.shape[0]
    group_devices = repeats // local_heads
    group_index = lax.axis_index("sp") * local_heads // repeats
    value_proj = (
        jnp.dot(prompt_token_rows, content_mapping_matrix, preferred_element_type=jnp.float32)
        .astype(jnp.bfloat16)
        .reshape(span_len, HEADS, HEAD)
    )
    key_proj = (
        jnp.dot(prompt_token_rows, address_mapping_matrix, preferred_element_type=jnp.float32)
        .astype(jnp.bfloat16)
        .reshape(span_len, GROUPS, STATE)
    )
    rate_raw = jnp.dot(
        prompt_token_rows, increment_mapping_matrix, preferred_element_type=jnp.float32
    ).astype(jnp.bfloat16)
    key_copies = jnp.repeat(key_proj, repeats, axis=1)
    value_seq, key_seq, rate_seq = (
        lax.all_to_all(value_proj, "sp", split_axis=1, concat_axis=0, tiled=True),
        lax.all_to_all(key_copies, "sp", split_axis=1, concat_axis=0, tiled=True),
        lax.all_to_all(rate_raw, "sp", split_axis=1, concat_axis=0, tiled=True),
    )
    key_group = key_seq[:, 0:1]
    seq_len = value_seq.shape[0]
    kernel_key = lax.dynamic_slice_in_dim(address_smoothing_coefficients, group_index, 1, 1)
    value_conv = jax.nn.silu(
        centred(value_seq.astype(jnp.float32), content_smoothing_coefficients)
    ).astype(jnp.bfloat16)
    key_conv = jax.nn.silu(centred(key_group.astype(jnp.float32), kernel_key)).astype(jnp.bfloat16)
    key_heads = jnp.broadcast_to(key_conv, (seq_len, local_heads, STATE))
    smoothed_increment_speed = jax.nn.softplus(
        rate_seq.astype(jnp.float32) + increment_speed_offset
    )
    exponent_increment_amount = (
        -jnp.exp(channel_fading_exponent) * smoothed_increment_speed + extra_damping_spikes[0].T
    )
    cumul = jnp.cumsum(exponent_increment_amount, axis=0)
    end_weight = jnp.exp(cumul[-1] - cumul)
    weighted = (
        value_conv.astype(jnp.float32) * (smoothed_increment_speed * end_weight)[:, :, None]
    ).astype(jnp.bfloat16)
    states = jnp.einsum("lhp,lhn->hpn", weighted, key_heads, preferred_element_type=jnp.float32)
    query_vector_row = lax.dynamic_slice_in_dim(newest_lookup_matrix[0], group_index, 1, 0).astype(
        jnp.float32
    )
    query_heads = jnp.broadcast_to(query_vector_row, (local_heads, STATE))
    raw_read = jnp.einsum("hpn,hn->hp", states, query_heads, precision=lax.Precision.HIGHEST)
    gated_read = raw_read * jax.nn.silu(newest_output_switch[0].astype(jnp.float32))
    group_sq = jnp.sum(gated_read * gated_read).reshape(1)
    for level in range(group_devices.bit_length() - 1):
        group_sq = group_sq + swapped(group_sq, "sp", level)
    scaled = (
        gated_read * lax.rsqrt(group_sq[0] / (repeats * HEAD) + EPS) * cluster_scaling_coefficients
    )
    kv_rows = jnp.concatenate([value_conv, key_heads], axis=-1)
    return (kv_rows[None], scaled.astype(jnp.bfloat16)[None])


XLANES = 128
HALO = 16
INNER = (2, 0, 1, 3)
OUTER = (1, 0, 2, 3)
INNER_KEYS = (3, 2, 1)
OUTER_KEYS = (1, 2, 3)
MESH = pl.DeviceIdType.MESH


def flipped(index, inner, outer):
    low, high = index % 2, (index // 2) % 2
    inside = low + high - 2 * low * high
    total = 0
    for bit, digit in enumerate((low, high)):
        flip = inside * ((inner >> bit) & 1) + (1 - inside) * ((outer >> bit) & 1)
        total = total + 2**bit * (digit + flip - 2 * digit * flip)
    return total


def mixer_kernel(
    n,
    x_hbm,
    wv_hbm,
    wk_hbm,
    wr_hbm,
    offset_hbm,
    fade_hbm,
    spikes_hbm,
    taps_hbm,
    key_taps_hbm,
    query_hbm,
    gate_hbm,
    gain_hbm,
    rows_out,
    read_out,
    wr_ref,
    offset_ref,
    fade_ref,
    spikes_ref,
    taps_ref,
    key_taps_ref,
    query_ref,
    gate_ref,
    gain_ref,
    small_sem,
    x_ext,
    wv,
    wk,
    proj,
    taps_all,
    key_send,
    key_recv,
    value_send,
    value_recv,
    rate_send,
    rate_recv,
    rate_rows,
    spike_rows,
    weights,
    acc,
    mixed,
    packed,
    square_send,
    square_recv,
    load_sem,
    halo_send_sem,
    halo_recv_sem,
    taps_send_sem,
    taps_recv_sem,
    rate_send_sem,
    rate_recv_sem,
    key_send_sem,
    key_recv_sem,
    forward_sem,
    value_send_sem,
    value_recv_sem,
    square_sem,
    out_sem,
):
    span = x_hbm.shape[0]
    half = span // 2
    rows_ext = span + 2 * HALO
    me = lax.axis_index("sp")
    z, y = me // 2, me % 2
    partner = 2 * z + 1 - y
    chunk = 128
    chunks = span // chunk

    def remote(src, dst, send, recv, device):
        return pltpu.make_async_remote_copy(
            src_ref=src,
            dst_ref=dst,
            send_sem=send,
            recv_sem=recv,
            device_id={"sp": device},
            device_id_type=MESH,
        )

    small = []
    for index, (source, target) in enumerate(
        (
            (taps_hbm, taps_ref),
            (key_taps_hbm, key_taps_ref),
            (wr_hbm, wr_ref),
            (offset_hbm, offset_ref),
            (fade_hbm, fade_ref),
            (spikes_hbm, spikes_ref),
            (query_hbm, query_ref),
            (gate_hbm, gate_ref),
            (gain_hbm, gain_ref),
        )
    ):
        small.append(pltpu.make_async_copy(source, target, small_sem.at[index]))
    small[0].start()
    load_x = [
        pltpu.make_async_copy(
            x_hbm.at[pl.ds(part * half, half)],
            x_ext.at[pl.ds(HALO + part * half, half)],
            load_sem.at[6 * part],
        )
        for part in range(2)
    ]
    load_k = pltpu.make_async_copy(wk_hbm, wk, load_sem.at[1])
    load_k.start()
    load_x[0].start()
    load_x[1].start()
    groups = [flipped(z, inner, outer) for inner, outer in zip(INNER, OUTER)]
    key_groups = [flipped(z, inner, outer) for inner, outer in zip(INNER_KEYS, OUTER_KEYS)]
    own_step = INNER.index(0)
    load_v = []
    for step, group in enumerate(groups):
        columns = pl.ds(pl.multiple_of(group * 256, 256), 256)
        load_v.append(
            pltpu.make_async_copy(wv_hbm.at[:, columns], wv.at[step], load_sem.at[2 + step])
        )
        load_v[-1].start()
    for copy in small[1:]:
        copy.start()

    barrier = pltpu.get_barrier_semaphore()
    for hop in range(1, n):
        pl.semaphore_signal(
            barrier, inc=1, device_id={"sp": (me + hop) % n}, device_id_type=MESH
        )
    small[0].wait()
    own_taps = jnp.concatenate([taps_ref[:, 0, :], taps_ref[:, 1, :]], axis=1)
    taps_all[me] = jnp.concatenate([own_taps, jnp.zeros((3, XLANES), jnp.float32)], axis=0)
    pl.semaphore_wait(barrier, n - 1)

    copies = []
    after, before = (me + 1) % n, (me + n - 1) % n
    halo_down = remote(
        x_hbm.at[pl.ds(span - HALO, HALO)],
        x_ext.at[pl.ds(0, HALO)],
        halo_send_sem.at[0],
        halo_recv_sem.at[0],
        after,
    )
    halo_up = remote(
        x_hbm.at[pl.ds(0, HALO)],
        x_ext.at[pl.ds(span + HALO, HALO)],
        halo_send_sem.at[1],
        halo_recv_sem.at[1],
        before,
    )
    halo_down.start()
    halo_up.start()
    for hop in range(1, n):
        copy = remote(
            taps_all.at[me],
            taps_all.at[me],
            taps_send_sem.at[hop],
            taps_recv_sem.at[me],
            (me + hop) % n,
        )
        copy.start()
        copies.append(copy)

    piece = rows_ext // 2

    def project_rows(weight, rows):
        proj[rows, :] = (
            jnp.dot(x_ext[rows, :], weight[...], preferred_element_type=jnp.float32)
            .astype(jnp.bfloat16)
            .astype(jnp.float32)
        )

    def project(weight):
        @pl.loop(0, 2)
        def _(index):
            project_rows(weight, pl.ds(pl.multiple_of(index * piece, 16), piece))

    def smooth(index, taps):
        window = proj[pl.ds(pl.multiple_of(index * chunk + 8, 8), chunk + 16), :]
        summed = taps[0:1] * window[6 : 6 + chunk]
        for tap in range(1, KERNEL):
            summed = summed + taps[tap : tap + 1] * window[6 + tap : 6 + tap + chunk]
        return summed * jax.nn.sigmoid(summed)

    load_k.wait()
    load_x[0].wait()
    halo_down.wait_recv()

    @pl.when(me == 0)
    def _():
        x_ext[0:HALO, :] = jnp.zeros((HALO, x_ext.shape[1]), jnp.bfloat16)

    project_rows(wk, pl.ds(0, piece))
    load_x[1].wait()
    halo_up.wait_recv()

    @pl.when(me == n - 1)
    def _():
        x_ext[span + HALO :, :] = jnp.zeros((HALO, x_ext.shape[1]), jnp.bfloat16)

    project_rows(wk, pl.ds(piece, piece))
    small[1].wait()
    key_taps = jnp.concatenate([key_taps_ref[:, g, :] for g in range(GROUPS)], axis=1)
    lane = lax.broadcasted_iota(jnp.int32, (chunk, XLANES), 1)

    @pl.loop(0, chunks // 2)
    def _(index):
        first = smooth(index, key_taps)
        second = smooth(index + chunks // 2, key_taps)
        rows = pl.ds(pl.multiple_of(index * chunk, chunk), chunk)
        for pair in range(2):
            low = first[:, pair * XLANES : (pair + 1) * XLANES]
            high = second[:, pair * XLANES : (pair + 1) * XLANES]
            key_send[2 * pair, rows, :] = jnp.where(
                lane < 64, low, pltpu.roll(high, 64, 1)
            ).astype(jnp.bfloat16)
            key_send[2 * pair + 1, rows, :] = jnp.where(
                lane < 64, pltpu.roll(low, 64, 1), high
            ).astype(jnp.bfloat16)

    for step in range(3):
        copy = remote(
            key_send.at[key_groups[step]],
            key_recv.at[me],
            key_send_sem.at[step],
            key_recv_sem.at[me],
            2 * key_groups[step] + y,
        )
        copy.start()
        copies.append(copy)
    own_forward = remote(
        key_send.at[z], key_recv.at[me], forward_sem.at[3], key_recv_sem.at[me], partner
    )
    own_forward.start()
    copies.append(own_forward)
    key_recv[me] = key_send[z]

    for hop in range(1, n):
        source = (me + hop) % n
        remote(
            taps_all.at[source],
            taps_all.at[source],
            taps_send_sem.at[hop],
            taps_recv_sem.at[source],
            source,
        ).wait_recv()

    def send_rates():
        small[2].wait()
        raw = lax.dot_general(
            wr_ref[...],
            x_ext[HALO : HALO + span, :],
            (((1,), (1,)), ((), ())),
            preferred_element_type=jnp.float32,
        )
        raw = raw.astype(jnp.bfloat16).astype(jnp.float32)
        for device in range(n):
            rate_send[device] = raw[2 * device : 2 * device + 2]
        rate_recv[me] = rate_send[me]
        for hop in range(1, n):
            other = (me + hop) % n
            copy = remote(
                rate_send.at[other],
                rate_recv.at[me],
                rate_send_sem.at[hop],
                rate_recv_sem.at[me],
                other,
            )
            copy.start()
            copies.append(copy)

    def key_wait(source):
        remote(
            key_recv.at[source],
            key_recv.at[source],
            forward_sem.at[0],
            key_recv_sem.at[source],
            partner,
        ).wait_recv()

    def forward_keys():
        for step in range(3):
            source = 2 * key_groups[step] + y
            key_wait(source)
            copy = remote(
                key_recv.at[source],
                key_recv.at[source],
                forward_sem.at[step],
                key_recv_sem.at[source],
                partner,
            )
            copy.start()
            copies.append(copy)

    for step, group in enumerate(groups):
        load_v[step].wait()
        project(wv.at[step])
        taps = jnp.concatenate([taps_all[2 * group], taps_all[2 * group + 1]], axis=1)

        @pl.loop(0, chunks)
        def _(index):
            value = smooth(index, taps).astype(jnp.bfloat16)
            rows = pl.ds(pl.multiple_of(index * chunk, chunk), chunk)
            value_send[step, 0, rows, :] = value[:, :XLANES]
            value_send[step, 1, rows, :] = value[:, XLANES:]

        if step == own_step:
            copy = remote(
                value_send.at[step, 1 - y],
                value_recv.at[me],
                value_send_sem.at[step, 0],
                value_recv_sem.at[me],
                partner,
            )
            copy.start()
            copies.append(copy)
            value_recv[me] = value_send[step, y]
        else:
            for side in range(2):
                copy = remote(
                    value_send.at[step, side],
                    value_recv.at[me],
                    value_send_sem.at[step, side],
                    value_recv_sem.at[me],
                    2 * group + side,
                )
                copy.start()
                copies.append(copy)
        if step == 0:
            send_rates()
        if step == 2:
            forward_keys()
    for wanted in small[3:]:
        wanted.wait()
    for hop in range(1, n):
        source = (me + hop) % n
        remote(
            rate_send.at[source],
            rate_recv.at[source],
            rate_send_sem.at[hop],
            rate_recv_sem.at[source],
            source,
        ).wait_recv()
    for source in range(n):
        rate_rows[2 * source : 2 * source + 2, :] = rate_recv[source]
        spike_rows[2 * source : 2 * source + 2, :] = spikes_ref[
            :, source * span : (source + 1) * span
        ]
    full = (2 * n, span)
    odd = lax.broadcasted_iota(jnp.int32, full, 0) % 2 == 1
    position = lax.broadcasted_iota(jnp.int32, full, 1)
    shifted = rate_rows[...] + jnp.where(odd, offset_ref[0:1, 1:2], offset_ref[0:1, 0:1])
    rate = jnp.maximum(shifted, 0.0) + jnp.log1p(jnp.exp(-jnp.abs(shifted)))
    decay = jnp.exp(jnp.where(odd, fade_ref[0:1, 1:2], fade_ref[0:1, 0:1]))
    later = spike_rows[...] - decay * rate
    reach = 1
    while reach < span:
        later = later + jnp.where(
            position < span - reach, pltpu.roll(later, span - reach, 1), 0.0
        )
        reach *= 2
    blocks = jnp.broadcast_to(later[:, 0:1], (2 * n, XLANES))
    block_row = lax.broadcasted_iota(jnp.int32, (2 * n, XLANES), 0)
    reach = 2
    while reach < 2 * n:
        blocks = blocks + jnp.where(
            block_row < 2 * n - reach, pltpu.roll(blocks, 2 * n - reach, 0), 0.0
        )
        reach *= 2
    blocks = jnp.where(block_row < 2 * n - 2, pltpu.roll(blocks, 2 * n - 2, 0), 0.0)
    later = jnp.where(position < span - 1, pltpu.roll(later, span - 1, 1), 0.0)
    scaled = rate * jnp.exp(later + blocks[:, 0:1])
    for source in range(n):
        weights[source] = scaled[2 * source : 2 * source + 2]

    queries = query_ref[...].astype(jnp.float32)
    query_row = lax.broadcasted_iota(jnp.int32, queries.shape, 0)
    query = jnp.sum(jnp.where(query_row == z, queries, 0.0), axis=0, keepdims=True)
    blank = jnp.zeros((1, 64), jnp.float32)
    asked = jnp.concatenate(
        [
            jnp.concatenate([query, blank], axis=1),
            jnp.concatenate([blank, query], axis=1),
            jnp.zeros((6, XLANES), jnp.float32),
        ],
        axis=0,
    ).astype(jnp.bfloat16)
    acc[...] = jnp.zeros_like(acc)

    def read(source):
        scores = lax.dot_general(
            asked,
            key_recv[source],
            (((1,), (1,)), ((), ())),
            preferred_element_type=jnp.float32,
        )
        share = weights[source] * jnp.concatenate([scores[0:1], scores[1:2]], axis=1)
        high = share.astype(jnp.bfloat16).astype(jnp.float32)
        parts = jnp.concatenate(
            [high, share - high, jnp.zeros((4, span), jnp.float32)], axis=0
        ).astype(jnp.bfloat16)
        acc[...] += jnp.dot(parts, value_recv[source], preferred_element_type=jnp.float32)

    def assemble(source, slot):
        for part in range(2):

            @pl.loop(0, chunks // 2)
            def _(index):
                at = pl.multiple_of(index * chunk, chunk)
                value = value_recv[source, pl.ds(part * half + at, chunk), :].astype(jnp.float32)
                key = key_recv[source, pl.ds(at, chunk), :].astype(jnp.float32)
                if part == 0:
                    key = pltpu.roll(key, 64, 1)
                mixed[pl.ds(0, chunk, stride=2), :] = jnp.where(lane < 64, value, key)
                mixed[pl.ds(1, chunk, stride=2), :] = jnp.where(
                    lane < 64, pltpu.roll(value, 64, 1), key
                )
                packed[slot, pl.ds(2 * (part * half + at), 2 * chunk), :] = mixed[...].astype(
                    jnp.bfloat16
                )

        out = pltpu.make_async_copy(
            packed.at[slot],
            rows_out.at[pl.ds(pl.multiple_of(source * 2 * span, 2 * span), 2 * span)],
            out_sem.at[slot],
        )
        out.start()
        return out

    order = [(me, False, False), (partner, True, True)]
    for step in (2, 0, 3):
        order.append((2 * groups[step] + y, False, True))
        order.append((2 * groups[step] + 1 - y, True, True))
    outs = []
    for index, (source, wait_key, wait_value) in enumerate(order):
        if wait_key:
            key_wait(source)
        if wait_value:
            remote(
                value_recv.at[source],
                value_recv.at[source],
                value_send_sem.at[0, 0],
                value_recv_sem.at[source],
                source,
            ).wait_recv()
        read(source)
        if index < n - 1:
            if index >= 2:
                outs[index - 2].wait()
            outs.append(assemble(source, index % 2))

    total = acc[...]
    first, second = total[0:1] + total[2:3], total[1:2] + total[3:4]
    line = lax.broadcasted_iota(jnp.int32, (1, XLANES), 1)
    raw_read = jnp.where(line < 64, first, second)
    gate = gate_ref[...].astype(jnp.float32)
    gate = jnp.concatenate([gate[0:1], gate[1:2]], axis=1)
    gain = gain_ref[...]
    gain = jnp.concatenate([gain[0:1], gain[1:2]], axis=1)
    gated = raw_read * (gate * jax.nn.sigmoid(gate))
    square = jnp.sum(gated * gated, axis=1, keepdims=True)
    square_send[...] = jnp.broadcast_to(square, square_send.shape)
    swap = remote(square_send, square_recv, square_sem.at[0], square_sem.at[1], partner)
    swap.start()
    outs[n - 3].wait()
    outs.append(assemble(order[-1][0], (n - 1) % 2))
    swap.wait()
    both = square + square_recv[0:1, 0:1]
    result = gated * lax.rsqrt(both / (GROUP_HEADS * HEAD) + EPS) * gain
    read_out[0:1, :] = result[:, :64]
    read_out[1:2, :] = result[:, 64:]

    outs[-2].wait()
    outs[-1].wait()
    halo_down.wait_send()
    halo_up.wait_send()
    for copy in copies:
        copy.wait_send()


def on_device_kernel(n, *arguments):
    x, wv, wk, wr, offset, fade, spikes, taps, key_taps, query, gate, gain = arguments
    span, model = x.shape[1:]
    f32, bf16 = jnp.float32, jnp.bfloat16
    vmem = pl.BlockSpec(memory_space=pltpu.VMEM)
    anywhere = pl.BlockSpec(memory_space=pl.ANY)
    stored = pl.BlockSpec(memory_space=pltpu.HBM)
    small = (
        wr.T,
        offset.reshape(1, 2),
        fade.reshape(1, 2),
        spikes[0],
        taps,
        key_taps,
        query[0],
        gate[0],
        gain,
    )
    dma = pltpu.SemaphoreType.DMA
    rows, read = pl.pallas_call(
        functools.partial(mixer_kernel, n),
        out_shape=(
            jax.ShapeDtypeStruct((n * span * 2, 128), bf16),
            jax.ShapeDtypeStruct((2, HEAD), f32),
        ),
        in_specs=[stored] * (3 + len(small)),
        out_specs=(anywhere, vmem),
        scratch_shapes=[pltpu.VMEM(value.shape, value.dtype) for value in small]
        + [
            dma((len(small),)),
            pltpu.VMEM((span + 2 * HALO, model), bf16),
            pltpu.VMEM((4, model, 256), bf16),
            pltpu.VMEM((model, 256), bf16),
            pltpu.VMEM((span + 2 * HALO, 256), f32),
            pltpu.VMEM((n, 8, 128), f32),
            pltpu.VMEM((GROUPS, span // 2, 128), bf16),
            pltpu.VMEM((n, span // 2, 128), bf16),
            pltpu.VMEM((4, 2, span, 128), bf16),
            pltpu.VMEM((n, span, 128), bf16),
            pltpu.VMEM((n, 2, span), f32),
            pltpu.VMEM((n, 2, span), f32),
            pltpu.VMEM((2 * n, span), f32),
            pltpu.VMEM((2 * n, span), f32),
            pltpu.VMEM((n, 2, span), f32),
            pltpu.VMEM((8, 128), f32),
            pltpu.VMEM((256, 128), f32),
            pltpu.VMEM((2, 2 * span, 128), bf16),
            pltpu.VMEM((8, 128), f32),
            pltpu.VMEM((8, 128), f32),
            dma((7,)),
            dma((2,)),
            dma((2,)),
            dma((n,)),
            dma((n,)),
            dma((n,)),
            dma((n,)),
            dma((3,)),
            dma((n,)),
            dma((4,)),
            dma((4, 2)),
            dma((n,)),
            dma((2,)),
            dma((2,)),
        ],
        compiler_params=pltpu.CompilerParams(
            collective_id=0, has_side_effects=True, vmem_limit_bytes=61000000
        ),
    )(x[0], wv, wk, *small)
    return rows.reshape(1, n * span, 2, 2 * HEAD), read.astype(bf16)[None]


def solution(mesh):
    placed = (
        P(("gr", "tp"), "sp", None),
        P(),
        P(),
        P(),
        P("sp"),
        P("sp"),
        P(("gr", "tp"), "sp", None),
        P(None, "sp", None),
        P(),
        P(("gr", "tp"), None, None),
        P(("gr", "tp"), "sp", None),
        P("sp", None),
    )
    devices = mesh.shape["sp"]
    pairs = HEADS == 2 * devices and GROUPS * 2 == devices
    return jax.shard_map(
        functools.partial(on_device_kernel, devices) if pairs else on_device,
        mesh=mesh,
        in_specs=placed,
        out_specs=(P(("gr", "tp"), None, "sp", None), P(("gr", "tp"), "sp", None)),
        check_vma=False,
    )
```

```python
import functools

import jax
import jax.numpy as jnp
from jax import lax
from jax.experimental import pallas as pl
from jax.experimental.pallas import tpu as pltpu
from jax.sharding import PartitionSpec as P

HEADS = 16
HEAD = 64
GROUPS = 4
STATE = 64
KERNEL = 5
GROUP_HEADS = HEADS // GROUPS


EPS = 1e-05


def swapped(value, axis, bit):
    mask = 2**bit
    pairs = [(source, source ^ mask) for source in range(lax.axis_size(axis))]
    return lax.ppermute(value, axis, pairs)


def centred(signal, kernel):
    margin = kernel.shape[0] // 2
    length = signal.shape[0]
    padded = jnp.pad(signal, ((margin, margin), (0, 0), (0, 0)))
    summed = kernel[0] * padded[0:length]
    for offset in range(1, kernel.shape[0]):
        summed = summed + kernel[offset] * padded[offset : offset + length]
    return summed


def on_device(
    context_input_tensor,
    content_mapping_matrix,
    address_mapping_matrix,
    increment_mapping_matrix,
    increment_speed_offset,
    channel_fading_exponent,
    extra_damping_spikes,
    content_smoothing_coefficients,
    address_smoothing_coefficients,
    newest_lookup_matrix,
    newest_output_switch,
    cluster_scaling_coefficients,
):
    prompt_token_rows = context_input_tensor[0]
    span_len = prompt_token_rows.shape[0]
    repeats = HEADS // GROUPS
    local_heads = increment_speed_offset.shape[0]
    group_devices = repeats // local_heads
    group_index = lax.axis_index("sp") * local_heads // repeats
    value_proj = (
        jnp.dot(prompt_token_rows, content_mapping_matrix, preferred_element_type=jnp.float32)
        .astype(jnp.bfloat16)
        .reshape(span_len, HEADS, HEAD)
    )
    key_proj = (
        jnp.dot(prompt_token_rows, address_mapping_matrix, preferred_element_type=jnp.float32)
        .astype(jnp.bfloat16)
        .reshape(span_len, GROUPS, STATE)
    )
    rate_raw = jnp.dot(
        prompt_token_rows, increment_mapping_matrix, preferred_element_type=jnp.float32
    ).astype(jnp.bfloat16)
    key_copies = jnp.repeat(key_proj, repeats, axis=1)
    value_seq, key_seq, rate_seq = (
        lax.all_to_all(value_proj, "sp", split_axis=1, concat_axis=0, tiled=True),
        lax.all_to_all(key_copies, "sp", split_axis=1, concat_axis=0, tiled=True),
        lax.all_to_all(rate_raw, "sp", split_axis=1, concat_axis=0, tiled=True),
    )
    key_group = key_seq[:, 0:1]
    seq_len = value_seq.shape[0]
    kernel_key = lax.dynamic_slice_in_dim(address_smoothing_coefficients, group_index, 1, 1)
    value_conv = jax.nn.silu(
        centred(value_seq.astype(jnp.float32), content_smoothing_coefficients)
    ).astype(jnp.bfloat16)
    key_conv = jax.nn.silu(centred(key_group.astype(jnp.float32), kernel_key)).astype(jnp.bfloat16)
    key_heads = jnp.broadcast_to(key_conv, (seq_len, local_heads, STATE))
    smoothed_increment_speed = jax.nn.softplus(
        rate_seq.astype(jnp.float32) + increment_speed_offset
    )
    exponent_increment_amount = (
        -jnp.exp(channel_fading_exponent) * smoothed_increment_speed + extra_damping_spikes[0].T
    )
    cumul = jnp.cumsum(exponent_increment_amount, axis=0)
    end_weight = jnp.exp(cumul[-1] - cumul)
    weighted = (
        value_conv.astype(jnp.float32) * (smoothed_increment_speed * end_weight)[:, :, None]
    ).astype(jnp.bfloat16)
    states = jnp.einsum("lhp,lhn->hpn", weighted, key_heads, preferred_element_type=jnp.float32)
    query_vector_row = lax.dynamic_slice_in_dim(newest_lookup_matrix[0], group_index, 1, 0).astype(
        jnp.float32
    )
    query_heads = jnp.broadcast_to(query_vector_row, (local_heads, STATE))
    raw_read = jnp.einsum("hpn,hn->hp", states, query_heads, precision=lax.Precision.HIGHEST)
    gated_read = raw_read * jax.nn.silu(newest_output_switch[0].astype(jnp.float32))
    group_sq = jnp.sum(gated_read * gated_read).reshape(1)
    for level in range(group_devices.bit_length() - 1):
        group_sq = group_sq + swapped(group_sq, "sp", level)
    scaled = (
        gated_read * lax.rsqrt(group_sq[0] / (repeats * HEAD) + EPS) * cluster_scaling_coefficients
    )
    kv_rows = jnp.concatenate([value_conv, key_heads], axis=-1)
    return (kv_rows[None], scaled.astype(jnp.bfloat16)[None])


XLANES = 128
HALO = 16
INNER = (2, 0, 1, 3)
OUTER = (1, 0, 2, 3)
ARRIVALS = (2, 0, 3)
FORWARD_STEP = 2
INNER_KEYS = (3, 2, 1)
OUTER_KEYS = (1, 2, 3)
MESH = pl.DeviceIdType.MESH


def flipped(index, inner, outer):
    low, high = index % 2, (index // 2) % 2
    inside = low + high - 2 * low * high
    total = 0
    for bit, digit in enumerate((low, high)):
        flip = inside * ((inner >> bit) & 1) + (1 - inside) * ((outer >> bit) & 1)
        total = total + 2**bit * (digit + flip - 2 * digit * flip)
    return total


def mixer_kernel(
    n,
    x_hbm,
    wv_hbm,
    wk_hbm,
    wr_hbm,
    offset_hbm,
    fade_hbm,
    spikes_hbm,
    taps_hbm,
    key_taps_hbm,
    query_hbm,
    gate_hbm,
    gain_hbm,
    rows_out,
    read_out,
    wr_ref,
    offset_ref,
    fade_ref,
    spikes_ref,
    taps_ref,
    key_taps_ref,
    query_ref,
    gate_ref,
    gain_ref,
    small_sem,
    x_ext,
    wv,
    wk,
    proj,
    taps_all,
    key_send,
    key_recv,
    value_send,
    value_recv,
    rate_send,
    rate_recv,
    rate_rows,
    spike_rows,
    weights,
    acc,
    mixed,
    square_send,
    square_recv,
    load_sem,
    halo_send_sem,
    halo_recv_sem,
    taps_send_sem,
    taps_recv_sem,
    rate_send_sem,
    rate_recv_sem,
    key_send_sem,
    key_recv_sem,
    forward_sem,
    value_send_sem,
    value_recv_sem,
    square_sem,
):
    span = x_hbm.shape[0]
    half = span // 2
    rows_ext = span + 2 * HALO
    me = lax.axis_index("sp")
    z, y = me // 2, me % 2
    partner = 2 * z + 1 - y
    chunk = 128
    chunks = span // chunk

    def remote(src, dst, send, recv, device):
        return pltpu.make_async_remote_copy(
            src_ref=src,
            dst_ref=dst,
            send_sem=send,
            recv_sem=recv,
            device_id={"sp": device},
            device_id_type=MESH,
        )

    small = []
    for index, (source, target) in enumerate(
        (
            (taps_hbm, taps_ref),
            (key_taps_hbm, key_taps_ref),
            (wr_hbm, wr_ref),
            (offset_hbm, offset_ref),
            (fade_hbm, fade_ref),
            (spikes_hbm, spikes_ref),
            (query_hbm, query_ref),
            (gate_hbm, gate_ref),
            (gain_hbm, gain_ref),
        )
    ):
        small.append(pltpu.make_async_copy(source, target, small_sem.at[index]))
    small[0].start()
    load_x = [
        pltpu.make_async_copy(
            x_hbm.at[pl.ds(part * half, half)],
            x_ext.at[pl.ds(HALO + part * half, half)],
            load_sem.at[6 * part],
        )
        for part in range(2)
    ]
    load_k = pltpu.make_async_copy(wk_hbm, wk, load_sem.at[1])
    load_k.start()
    load_x[0].start()
    load_x[1].start()
    groups = [flipped(z, inner, outer) for inner, outer in zip(INNER, OUTER)]
    key_groups = [flipped(z, inner, outer) for inner, outer in zip(INNER_KEYS, OUTER_KEYS)]
    own_step = INNER.index(0)
    load_v = []
    for step, group in enumerate(groups):
        columns = pl.ds(pl.multiple_of(group * 256, 256), 256)
        load_v.append(
            pltpu.make_async_copy(wv_hbm.at[:, columns], wv.at[step], load_sem.at[2 + step])
        )
        load_v[-1].start()
    for copy in small[1:]:
        copy.start()

    barrier = pltpu.get_barrier_semaphore()
    for hop in range(1, n):
        pl.semaphore_signal(
            barrier, inc=1, device_id={"sp": (me + hop) % n}, device_id_type=MESH
        )
    small[0].wait()
    own_taps = jnp.concatenate([taps_ref[:, 0, :], taps_ref[:, 1, :]], axis=1)
    taps_all[me] = jnp.concatenate([own_taps, jnp.zeros((3, XLANES), jnp.float32)], axis=0)
    pl.semaphore_wait(barrier, n - 1)

    copies = []
    after, before = (me + 1) % n, (me + n - 1) % n
    halo_down = remote(
        x_hbm.at[pl.ds(span - HALO, HALO)],
        x_ext.at[pl.ds(0, HALO)],
        halo_send_sem.at[0],
        halo_recv_sem.at[0],
        after,
    )
    halo_up = remote(
        x_hbm.at[pl.ds(0, HALO)],
        x_ext.at[pl.ds(span + HALO, HALO)],
        halo_send_sem.at[1],
        halo_recv_sem.at[1],
        before,
    )
    halo_down.start()
    halo_up.start()
    for hop in range(1, n):
        copy = remote(
            taps_all.at[me],
            taps_all.at[me],
            taps_send_sem.at[hop],
            taps_recv_sem.at[me],
            (me + hop) % n,
        )
        copy.start()
        copies.append(copy)

    piece = rows_ext // 2

    def project_rows(weight, rows):
        proj[rows, :] = (
            jnp.dot(x_ext[rows, :], weight[...], preferred_element_type=jnp.float32)
            .astype(jnp.bfloat16)
            .astype(jnp.float32)
        )

    def project(weight):
        @pl.loop(0, 2)
        def _(index):
            project_rows(weight, pl.ds(pl.multiple_of(index * piece, 16), piece))

    def smooth(index, taps):
        window = proj[pl.ds(pl.multiple_of(index * chunk + 8, 8), chunk + 16), :]
        summed = taps[0:1] * window[6 : 6 + chunk]
        for tap in range(1, KERNEL):
            summed = summed + taps[tap : tap + 1] * window[6 + tap : 6 + tap + chunk]
        return summed * jax.nn.sigmoid(summed)

    load_k.wait()
    load_x[0].wait()
    halo_down.wait_recv()

    @pl.when(me == 0)
    def _():
        x_ext[0:HALO, :] = jnp.zeros((HALO, x_ext.shape[1]), jnp.bfloat16)

    project_rows(wk, pl.ds(0, piece))
    load_x[1].wait()
    halo_up.wait_recv()

    @pl.when(me == n - 1)
    def _():
        x_ext[span + HALO :, :] = jnp.zeros((HALO, x_ext.shape[1]), jnp.bfloat16)

    project_rows(wk, pl.ds(piece, piece))
    small[1].wait()
    key_taps = jnp.concatenate([key_taps_ref[:, g, :] for g in range(GROUPS)], axis=1)
    lane = lax.broadcasted_iota(jnp.int32, (chunk, XLANES), 1)

    @pl.loop(0, chunks // 2)
    def _(index):
        first = smooth(index, key_taps)
        second = smooth(index + chunks // 2, key_taps)
        rows = pl.ds(pl.multiple_of(index * chunk, chunk), chunk)
        for pair in range(2):
            low = first[:, pair * XLANES : (pair + 1) * XLANES]
            high = second[:, pair * XLANES : (pair + 1) * XLANES]
            key_send[2 * pair, rows, :] = jnp.where(
                lane < 64, low, pltpu.roll(high, 64, 1)
            ).astype(jnp.bfloat16)
            key_send[2 * pair + 1, rows, :] = jnp.where(
                lane < 64, pltpu.roll(low, 64, 1), high
            ).astype(jnp.bfloat16)

    for step in range(3):
        copy = remote(
            key_send.at[key_groups[step]],
            key_recv.at[me],
            key_send_sem.at[step],
            key_recv_sem.at[me],
            2 * key_groups[step] + y,
        )
        copy.start()
        copies.append(copy)
    own_forward = remote(
        key_send.at[z], key_recv.at[me], forward_sem.at[3], key_recv_sem.at[me], partner
    )
    own_forward.start()
    copies.append(own_forward)
    key_recv[me] = key_send[z]

    for hop in range(1, n):
        source = (me + hop) % n
        remote(
            taps_all.at[source],
            taps_all.at[source],
            taps_send_sem.at[hop],
            taps_recv_sem.at[source],
            source,
        ).wait_recv()

    def send_rates():
        small[2].wait()
        raw = lax.dot_general(
            wr_ref[...],
            x_ext[HALO : HALO + span, :],
            (((1,), (1,)), ((), ())),
            preferred_element_type=jnp.float32,
        )
        raw = raw.astype(jnp.bfloat16).astype(jnp.float32)
        for device in range(n):
            rate_send[device] = raw[2 * device : 2 * device + 2]
        rate_recv[me] = rate_send[me]
        for hop in range(1, n):
            other = (me + hop) % n
            copy = remote(
                rate_send.at[other],
                rate_recv.at[me],
                rate_send_sem.at[hop],
                rate_recv_sem.at[me],
                other,
            )
            copy.start()
            copies.append(copy)

    def key_wait(source):
        remote(
            key_recv.at[source],
            key_recv.at[source],
            forward_sem.at[0],
            key_recv_sem.at[source],
            partner,
        ).wait_recv()

    def forward_keys():
        for step in range(3):
            source = 2 * key_groups[step] + y
            key_wait(source)
            copy = remote(
                key_recv.at[source],
                key_recv.at[source],
                forward_sem.at[step],
                key_recv_sem.at[source],
                partner,
            )
            copy.start()
            copies.append(copy)

    for step, group in enumerate(groups):
        load_v[step].wait()
        project(wv.at[step])
        taps = jnp.concatenate([taps_all[2 * group], taps_all[2 * group + 1]], axis=1)

        @pl.loop(0, chunks)
        def _(index):
            value = smooth(index, taps).astype(jnp.bfloat16)
            rows = pl.ds(pl.multiple_of(index * chunk, chunk), chunk)
            value_send[step, 0, rows, :] = value[:, :XLANES]
            value_send[step, 1, rows, :] = value[:, XLANES:]

        if step == own_step:
            copy = remote(
                value_send.at[step, 1 - y],
                value_recv.at[me],
                value_send_sem.at[step, 0],
                value_recv_sem.at[me],
                partner,
            )
            copy.start()
            copies.append(copy)
            value_recv[me] = value_send[step, y]
        else:
            for side in range(2):
                copy = remote(
                    value_send.at[step, (y + side) % 2],
                    value_recv.at[me],
                    value_send_sem.at[step, side],
                    value_recv_sem.at[me],
                    2 * group + (y + side) % 2,
                )
                copy.start()
                copies.append(copy)
        if step == 0:
            send_rates()
        if step == FORWARD_STEP:
            forward_keys()
    for wanted in small[3:]:
        wanted.wait()
    for hop in range(1, n):
        source = (me + hop) % n
        remote(
            rate_send.at[source],
            rate_recv.at[source],
            rate_send_sem.at[hop],
            rate_recv_sem.at[source],
            source,
        ).wait_recv()
    for source in range(n):
        rate_rows[2 * source : 2 * source + 2, :] = rate_recv[source]
        spike_rows[2 * source : 2 * source + 2, :] = spikes_ref[
            :, source * span : (source + 1) * span
        ]
    full = (2 * n, span)
    odd = lax.broadcasted_iota(jnp.int32, full, 0) % 2 == 1
    position = lax.broadcasted_iota(jnp.int32, full, 1)
    shifted = rate_rows[...] + jnp.where(odd, offset_ref[0:1, 1:2], offset_ref[0:1, 0:1])
    rate = jnp.maximum(shifted, 0.0) + jnp.log1p(jnp.exp(-jnp.abs(shifted)))
    decay = jnp.exp(jnp.where(odd, fade_ref[0:1, 1:2], fade_ref[0:1, 0:1]))
    later = spike_rows[...] - decay * rate
    reach = 1
    while reach < span:
        later = later + jnp.where(
            position < span - reach, pltpu.roll(later, span - reach, 1), 0.0
        )
        reach *= 2
    blocks = jnp.broadcast_to(later[:, 0:1], (2 * n, XLANES))
    block_row = lax.broadcasted_iota(jnp.int32, (2 * n, XLANES), 0)
    reach = 2
    while reach < 2 * n:
        blocks = blocks + jnp.where(
            block_row < 2 * n - reach, pltpu.roll(blocks, 2 * n - reach, 0), 0.0
        )
        reach *= 2
    blocks = jnp.where(block_row < 2 * n - 2, pltpu.roll(blocks, 2 * n - 2, 0), 0.0)
    later = jnp.where(position < span - 1, pltpu.roll(later, span - 1, 1), 0.0)
    scaled = rate * jnp.exp(later + blocks[:, 0:1])
    for source in range(n):
        weights[source] = scaled[2 * source : 2 * source + 2]

    queries = query_ref[...].astype(jnp.float32)
    query_row = lax.broadcasted_iota(jnp.int32, queries.shape, 0)
    query = jnp.sum(jnp.where(query_row == z, queries, 0.0), axis=0, keepdims=True)
    blank = jnp.zeros((1, 64), jnp.float32)
    asked = jnp.concatenate(
        [
            jnp.concatenate([query, blank], axis=1),
            jnp.concatenate([blank, query], axis=1),
            jnp.zeros((6, XLANES), jnp.float32),
        ],
        axis=0,
    ).astype(jnp.bfloat16)
    acc[...] = jnp.zeros_like(acc)

    def read(source):
        scores = lax.dot_general(
            asked,
            key_recv[source],
            (((1,), (1,)), ((), ())),
            preferred_element_type=jnp.float32,
        )
        share = weights[source] * jnp.concatenate([scores[0:1], scores[1:2]], axis=1)
        high = share.astype(jnp.bfloat16).astype(jnp.float32)
        parts = jnp.concatenate(
            [high, share - high, jnp.zeros((4, span), jnp.float32)], axis=0
        ).astype(jnp.bfloat16)
        acc[...] += jnp.dot(parts, value_recv[source], preferred_element_type=jnp.float32)

    def assemble(source):
        for part in range(2):

            @pl.loop(0, chunks // 2)
            def _(index):
                at = pl.multiple_of(index * chunk, chunk)
                value = value_recv[source, pl.ds(part * half + at, chunk), :].astype(jnp.float32)
                key = key_recv[source, pl.ds(at, chunk), :].astype(jnp.float32)
                if part == 0:
                    key = pltpu.roll(key, 64, 1)
                mixed[pl.ds(0, chunk, stride=2), :] = jnp.where(lane < 64, value, key)
                mixed[pl.ds(1, chunk, stride=2), :] = jnp.where(
                    lane < 64, pltpu.roll(value, 64, 1), key
                )
                line = pl.multiple_of(2 * (source * span + part * half + at), 2 * chunk)
                rows_out[pl.ds(line, 2 * chunk), :] = mixed[...].astype(jnp.bfloat16)

    order = [(me, False, False), (partner, True, True)]
    for step in ARRIVALS:
        order.append((2 * groups[step] + y, False, True))
        order.append((2 * groups[step] + 1 - y, True, True))
    for index, (source, wait_key, wait_value) in enumerate(order):
        if wait_key:
            key_wait(source)
        if wait_value:
            remote(
                value_recv.at[source],
                value_recv.at[source],
                value_send_sem.at[0, 0],
                value_recv_sem.at[source],
                source,
            ).wait_recv()
        read(source)
        if index < n - 1:
            assemble(source)

    total = acc[...]
    first, second = total[0:1] + total[2:3], total[1:2] + total[3:4]
    line = lax.broadcasted_iota(jnp.int32, (1, XLANES), 1)
    raw_read = jnp.where(line < 64, first, second)
    gate = gate_ref[...].astype(jnp.float32)
    gate = jnp.concatenate([gate[0:1], gate[1:2]], axis=1)
    gain = gain_ref[...]
    gain = jnp.concatenate([gain[0:1], gain[1:2]], axis=1)
    gated = raw_read * (gate * jax.nn.sigmoid(gate))
    square = jnp.sum(gated * gated, axis=1, keepdims=True)
    square_send[...] = jnp.broadcast_to(square, square_send.shape)
    swap = remote(square_send, square_recv, square_sem.at[0], square_sem.at[1], partner)
    swap.start()
    assemble(order[-1][0])
    swap.wait()
    both = square + square_recv[0:1, 0:1]
    result = gated * lax.rsqrt(both / (GROUP_HEADS * HEAD) + EPS) * gain
    read_out[0:1, :] = result[:, :64]
    read_out[1:2, :] = result[:, 64:]

    halo_down.wait_send()
    halo_up.wait_send()
    for copy in copies:
        copy.wait_send()


def on_device_kernel(n, *arguments):
    x, wv, wk, wr, offset, fade, spikes, taps, key_taps, query, gate, gain = arguments
    span, model = x.shape[1:]
    f32, bf16 = jnp.float32, jnp.bfloat16
    vmem = pl.BlockSpec(memory_space=pltpu.VMEM)
    stored = pl.BlockSpec(memory_space=pltpu.HBM)
    small = (
        wr.T,
        offset.reshape(1, 2),
        fade.reshape(1, 2),
        spikes[0],
        taps,
        key_taps,
        query[0],
        gate[0],
        gain,
    )
    dma = pltpu.SemaphoreType.DMA
    rows, read = pl.pallas_call(
        functools.partial(mixer_kernel, n),
        out_shape=(
            pltpu.VMEM((n * span * 2, 128), bf16),
            pltpu.VMEM((2, HEAD), f32),
        ),
        in_specs=[stored] * (3 + len(small)),
        out_specs=(vmem, vmem),
        scratch_shapes=[pltpu.VMEM(value.shape, value.dtype) for value in small]
        + [
            dma((len(small),)),
            pltpu.VMEM((span + 2 * HALO, model), bf16),
            pltpu.VMEM((4, model, 256), bf16),
            pltpu.VMEM((model, 256), bf16),
            pltpu.VMEM((span + 2 * HALO, 256), f32),
            pltpu.VMEM((n, 8, 128), f32),
            pltpu.VMEM((GROUPS, span // 2, 128), bf16),
            pltpu.VMEM((n, span // 2, 128), bf16),
            pltpu.VMEM((4, 2, span, 128), bf16),
            pltpu.VMEM((n, span, 128), bf16),
            pltpu.VMEM((n, 2, span), f32),
            pltpu.VMEM((n, 2, span), f32),
            pltpu.VMEM((2 * n, span), f32),
            pltpu.VMEM((2 * n, span), f32),
            pltpu.VMEM((n, 2, span), f32),
            pltpu.VMEM((8, 128), f32),
            pltpu.VMEM((256, 128), f32),
            pltpu.VMEM((8, 128), f32),
            pltpu.VMEM((8, 128), f32),
            dma((7,)),
            dma((2,)),
            dma((2,)),
            dma((n,)),
            dma((n,)),
            dma((n,)),
            dma((n,)),
            dma((3,)),
            dma((n,)),
            dma((4,)),
            dma((4, 2)),
            dma((n,)),
            dma((2,)),
        ],
        compiler_params=pltpu.CompilerParams(
            collective_id=0, has_side_effects=True, vmem_limit_bytes=56 * 2**20
        ),
    )(x[0], wv, wk, *small)
    return rows.reshape(1, n * span, 2, 2 * HEAD), read.astype(bf16)[None]


def solution(mesh):
    placed = (
        P(("gr", "tp"), "sp", None),
        P(),
        P(),
        P(),
        P("sp"),
        P("sp"),
        P(("gr", "tp"), "sp", None),
        P(None, "sp", None),
        P(),
        P(("gr", "tp"), None, None),
        P(("gr", "tp"), "sp", None),
        P("sp", None),
    )
    devices = mesh.shape["sp"]
    pairs = HEADS == 2 * devices and GROUPS * 2 == devices
    return jax.shard_map(
        functools.partial(on_device_kernel, devices) if pairs else on_device,
        mesh=mesh,
        in_specs=placed,
        out_specs=(P(("gr", "tp"), None, "sp", None), P(("gr", "tp"), "sp", None)),
        check_vma=False,
    )
```
